32 devices in a mesh: grp: 2 (over y), ep: 4 (over z), tp: 4 (over x, core).
Axes of the slice: x: 2, y: 2, z: 4, core: 2. Of those that a mesh axis runs over, the one named last changes fastest.
Arguments:
- query_rows: bfloat16 [1536, 2048], P(('grp', 'ep'), 'tp'), parts along dimension 0, may hold values from -100 to 100
- projected_keys: bfloat16 [1536, 512], P(('grp', 'ep'), 'tp'), parts along dimension 0, may hold values from -100 to 100
- projected_values: bfloat16 [1536, 512], P(('grp', 'ep'), 'tp'), parts along dimension 0, may hold values from -6 to 6
- query_gain: float32 [128], replicated, may hold values from 0.3 to 6.5
- key_norm_gain: float32 [128], replicated, may hold values from 0.3 to 6.5
- out_proj: bfloat16 [2048, 2048], P('tp'), may hold values from -4 to 4
- mix_tokens: bfloat16 [4096, 2048], P(('grp', 'ep', 'tp')), parts along dimension 0, may hold values from -150 to 150
- norm_gain: float32 [2048], replicated, may hold values from 0.1 to 1.9
- expert_ids: int32 [4096, 2], P(('grp', 'ep', 'tp')), parts along dimension 0, may hold values from 0 to 3, all different within a row; in each aligned block of 128 rows (0 to 127, 128 to 255, ...) at most 96 rows name the same one
- expert_score: float32 [4096, 2], P(('grp', 'ep', 'tp')), parts along dimension 0, may hold values from -6 to 6
- gate_proj: bfloat16 [4, 2048, 2048], P('ep', None, 'tp'), may hold values from -0.125 to 0.125
- up_proj: bfloat16 [4, 2048, 2048], P('ep', None, 'tp'), may hold values from -0.125 to 0.125
- down_proj: bfloat16 [4, 2048, 2048], P('ep', 'tp'), may hold values from -0.125 to 0.125
Outputs:
- mixed_rows: bfloat16 [1536, 2048], P(('grp', 'ep', 'tp')), parts along dimension 0
- expert_out: bfloat16 [4096, 2048], P(('grp', 'ep', 'tp')), parts along dimension 0
The draws below stay inside these ranges and needn't reach their ends.
There are 2 independent parts, one for each index of `grp`. The reference program is written for one: setup_inputs(seed, part) draws one part's arguments, and reference() takes and returns one part's arrays. A program takes and returns all parts, laid end to end along the dimension named above; an argument that names none is the same for every part. Nothing has to cross between parts.
Inputs may be any that keep to these rules, and one draw needn't show every extreme that they name: `expert_ids`: each row names 2 different experts. Within the rows of one device (aligned blocks of 128 rows) no expert is named more than 96 times, and in every draw some device names some expert exactly 96 times.
All inputs are finite; a program needn't handle non-finite values.
Results may differ from the reference program's by a relative error of at most 0.014.
The reference program's roundings to bfloat16 on the way count: a program that leaves them out, or rounds other values in their place, can miss the bound.
Values may be sent and summed in bfloat16 or wider, within the bound.
A program may use at most 128 MiB of HBM per device.

```python
import math
import jax
import jax.numpy as jnp
import numpy as np
from jax import lax

D = 2048
HEAD_SIZE = 128
QUERY_HEADS = 16
KEY_VALUE_HEADS = 4
GRID_W = 64
FFE = 2048
TOPK = 2
TOK_B_DEV = 128
EXPERTS = 4
ATTENTION_TOKENS = 768
TOKENS_B = 2048
CAP = 96
N_TP = 4


def attention_pair(key):
    folded = jax.random.fold_in(key, 11)
    keys_by_head = jax.random.split(folded, 4)
    query_matrix = jnp.clip(jax.random.normal(keys_by_head[0], (ATTENTION_TOKENS, QUERY_HEADS, HEAD_SIZE), jnp.float32), -5.0, 5.0)
    query_matrix = query_matrix * jnp.exp(jax.random.uniform(keys_by_head[1], (ATTENTION_TOKENS, QUERY_HEADS, 1), jnp.float32) * math.log(10.0))
    key_value_pairs = jnp.clip(jax.random.normal(keys_by_head[2], (ATTENTION_TOKENS, KEY_VALUE_HEADS, HEAD_SIZE), jnp.float32), -5.0, 5.0)
    key_value_pairs = key_value_pairs * jnp.exp(jax.random.uniform(keys_by_head[3], (ATTENTION_TOKENS, KEY_VALUE_HEADS, 1), jnp.float32) * math.log(10.0))
    query_matrix = jnp.clip(query_matrix, -100.0, 100.0).reshape(ATTENTION_TOKENS, QUERY_HEADS * HEAD_SIZE)
    key_value_pairs = jnp.clip(key_value_pairs, -100.0, 100.0).reshape(ATTENTION_TOKENS, KEY_VALUE_HEADS * HEAD_SIZE)
    return (query_matrix, key_value_pairs)


def draw_query_rows(key, part):
    return attention_pair(key)[0].astype(jnp.bfloat16)


def draw_projected_keys(key, part):
    return attention_pair(key)[1].astype(jnp.bfloat16)


def gain_draw(key):
    return jnp.clip(1.0 + 0.18 * jax.random.normal(key, (HEAD_SIZE,), jnp.float32), 0.3, 1.9)


def draw_query_gain(key, part):
    return gain_draw(jax.random.fold_in(key, 21))


def draw_key_norm_gain(key, part):
    return gain_draw(jax.random.fold_in(key, 22))


def draw_mix_tokens(key, part):
    keys_by_head = jax.random.split(jax.random.fold_in(key, 31), 3)
    row_scale = jnp.exp(jax.random.uniform(keys_by_head[1], (TOKENS_B, 1), jnp.float32) * math.log(10.0))
    col_scale = jnp.exp(jax.random.uniform(keys_by_head[2], (1, D), jnp.float32, math.log(0.3), math.log(3.0)))
    entries = jnp.clip(jax.random.normal(keys_by_head[0], (TOKENS_B, D), jnp.float32), -5.0, 5.0)
    return jnp.clip(entries * row_scale * col_scale, -150.0, 150.0).astype(jnp.bfloat16)


def level_of(stream_key, shape, shards, low, largest):
    level, own = 1.0, jax.random.fold_in(stream_key, 6)
    for axis_at, parts in shards:
        draws = jnp.exp(jax.random.uniform(jax.random.fold_in(own, axis_at), (parts,), jnp.float32, low / len(shards), largest / len(shards)))
        level = level * jnp.repeat(draws, shape[axis_at] // parts).reshape([-1 if axis == axis_at else 1 for axis in range(len(shape))])
    return level


def routed_block(stream_key, own, number, rows, count, top, most, lean):
    order = jax.random.permutation(stream_key, count)
    packed, usual = shares(count, rows * top, most, lean, True), shares(count, rows * top, most, lean, False)
    places = jnp.arange(count)

    def named(sizes, rotation):
        used = int((sizes > 0).sum())
        fixed = max(1, used // 4)
        moved = fixed + (places - fixed + rotation * (used - fixed)) % max(1, count - fixed)
        return jnp.zeros((count,), jnp.int32).at[order[jnp.where(places < fixed, places, moved)]].set(jnp.asarray(sizes, jnp.int32))

    sizes = jnp.where(number % 4 == 0, named(packed, number // 4), named(usual, number - number // 4 - 1))
    mixed = jax.random.permutation(jax.random.fold_in(own, 3), count)
    source_of, sink = mixed[0:count // 2 * 2:2], mixed[1:count // 2 * 2:2]
    room = jnp.minimum(sizes[source_of] - 1, most - sizes[sink]) // 2
    room = jnp.where((source_of == order[0]) | (sink == order[0]) | (sizes[sink] == 0), 0, jnp.maximum(room, 0))
    moved = jax.random.randint(jax.random.fold_in(own, 4), (count // 2,), 0, 1 << 20) % (room + 1)
    sizes = sizes.at[source_of].add(-moved).at[sink].add(moved)
    labels = jnp.searchsorted(jnp.cumsum(sizes), jnp.arange(rows * top), side="right").astype(jnp.int32)
    listing = labels.reshape(top, rows).T
    listing = listing[jax.random.permutation(jax.random.fold_in(own, 1), rows)]
    rotation = jax.random.randint(jax.random.fold_in(own, 2), (rows, 1), 0, top)
    return jnp.take_along_axis(listing, (jnp.arange(top)[None, :] + rotation) % top, axis=1)


def shares(amount, total, reach, slope, full):
    loads = [(1 << 20) // math.isqrt(rank ** slope) + 1 for rank in range(1, amount + 1)]
    largest = reach if full else min(reach, max(-(-total // amount), total * loads[0] // sum(loads)))
    least = 1 if total - largest >= amount - 1 else 0
    given, rest = [largest] + [least] * (amount - 1), total - largest - least * (amount - 1)
    while rest > 0:
        candidates = [i for i in range(1, amount) if given[i] < largest] or [i for i in range(1, amount) if given[i] < reach]
        pool, remaining = sum([loads[i] for i in candidates]), rest
        for i in candidates:
            extra = min(reach - given[i], max(1, remaining * loads[i] // pool), rest)
            given[i] = given[i] + extra
            rest = rest - extra
    return np.array(given)


def gaussian(stream_key, dims, deviation, bound, cuts=(), kind=jnp.bfloat16):
    result = deviation * jax.random.normal(stream_key, dims, jnp.float32)
    if cuts:
        result = result * level_of(stream_key, dims, cuts, -0.22, 0.18)
    return jnp.clip(result, -bound, bound).astype(kind)


def setup_inputs(seed: int = 0, part: int = 0) -> dict:
    keys = jax.random.split(jax.random.key(seed), 14)
    part_splits = jax.random.split(jax.random.fold_in(keys[13], part), 14)
    query_rows = draw_query_rows(jax.random.fold_in(jax.random.fold_in(keys[13], part), 71), part)
    projected_keys = draw_projected_keys(jax.random.fold_in(jax.random.fold_in(keys[13], part), 71), part)
    projected_values = gaussian(part_splits[2], (ATTENTION_TOKENS, KEY_VALUE_HEADS * HEAD_SIZE), 1.0, 6.0, ((0, 4), (1, 4)))
    query_gain = draw_query_gain(jax.random.fold_in(keys[13], 71), part)
    key_norm_gain = draw_key_norm_gain(jax.random.fold_in(keys[13], 71), part)
    out_proj = gaussian(keys[5], (QUERY_HEADS * HEAD_SIZE, D), (max(1, QUERY_HEADS * HEAD_SIZE // 1024)) ** -0.5, 4.0, ((0, 4),))
    mix_tokens = draw_mix_tokens(jax.random.fold_in(jax.random.fold_in(keys[13], part), 71), part)
    norm_gain = jnp.clip(1.0 + 0.18 * jax.random.normal(keys[7], (D,), jnp.float32), 0.1, 1.9)
    expert_ids_keys = jax.random.split(jax.random.fold_in(part_splits[8], 1), TOKENS_B // TOK_B_DEV)
    expert_ids_turns = jax.random.permutation(jax.random.fold_in(part_splits[8], 3), TOKENS_B // TOK_B_DEV)
    expert_ids = jax.vmap(lambda own, number: routed_block(jax.random.fold_in(part_splits[8], 2), own, number, TOK_B_DEV, EXPERTS, TOPK, CAP, 2))(expert_ids_keys, expert_ids_turns).reshape((TOKENS_B, TOPK))
    expert_score = gaussian(part_splits[9], (TOKENS_B, TOPK), 1.5, 6.0, ((0, 16),), jnp.float32)
    gate_proj = gaussian(keys[10], (EXPERTS, D, FFE), D ** -0.5, 0.125, ((0, 4), (2, 4)))
    up_proj = gaussian(keys[11], (EXPERTS, D, FFE), D ** -0.5, 0.125, ((0, 4), (2, 4)))
    down_proj = gaussian(keys[12], (EXPERTS, FFE, D), FFE ** -0.5, 0.125, ((0, 4), (1, 4)))
    return {"query_rows": query_rows, "projected_keys": projected_keys, "projected_values": projected_values, "query_gain": query_gain, "key_norm_gain": key_norm_gain, "out_proj": out_proj, "mix_tokens": mix_tokens, "norm_gain": norm_gain, "expert_ids": expert_ids, "expert_score": expert_score, "gate_proj": gate_proj, "up_proj": up_proj, "down_proj": down_proj}


EPS = 1e-06
THETA = 10000.0

def head_norm(vectors, gain):
    return vectors * lax.rsqrt(lax.optimization_barrier(jnp.mean(vectors * vectors, axis=-1, keepdims=True)) + EPS) * gain

def rotate_grid(vectors, token_positions):
    length, heads, head_dim = vectors.shape
    quarter = head_dim // 4
    freqs = 1.0 / THETA ** (jnp.arange(quarter, dtype=jnp.float32) * 4.0 / head_dim)
    grid_row = (token_positions // GRID_W).astype(jnp.float32)
    grid_col = (token_positions % GRID_W).astype(jnp.float32)
    angles = jnp.stack([grid_row[:, None] * freqs, grid_col[:, None] * freqs], axis=1)
    cosine = jnp.cos(angles)[:, None]
    sine = jnp.sin(angles)[:, None]
    halves = vectors.reshape(length, heads, 2, 2, quarter)
    first = halves[..., 0, :]
    second = halves[..., 1, :]
    turned = jnp.stack([first * cosine - second * sine, second * cosine + first * sine], axis=-2)
    return turned.reshape(length, heads, head_dim)

def prepare_inputs(raw_rows, gain, heads, token_positions):
    length = raw_rows.shape[0]
    vectors = raw_rows.astype(jnp.float32).reshape(length, heads, HEAD_SIZE)
    return rotate_grid(head_norm(vectors, gain), token_positions).astype(jnp.bfloat16)

def reference(query_rows, projected_keys, projected_values, query_gain, key_norm_gain, out_proj, mix_tokens, norm_gain, expert_ids, expert_score, gate_proj, up_proj, down_proj):
    token_total = query_rows.shape[0]
    token_positions = jnp.arange(token_total, dtype=jnp.int32)
    queries_per_group = QUERY_HEADS // KEY_VALUE_HEADS
    query_matrix = prepare_inputs(query_rows, query_gain, QUERY_HEADS, token_positions)
    keys_expanded = prepare_inputs(projected_keys, key_norm_gain, KEY_VALUE_HEADS, token_positions).astype(jnp.float32)
    values_expanded = projected_values.reshape(token_total, KEY_VALUE_HEADS, HEAD_SIZE).astype(jnp.float32)
    rows_per_block = math.gcd(token_total, 256)
    blocked_queries = query_matrix.reshape(token_total // rows_per_block, rows_per_block, KEY_VALUE_HEADS, queries_per_group, HEAD_SIZE)

    def attend(query_block):
        scores = jnp.einsum('tkgd,skd->kgts', query_block.astype(jnp.float32), keys_expanded) * HEAD_SIZE ** (-0.5)
        top_score = lax.optimization_barrier(jnp.max(scores, axis=-1, keepdims=True))
        probs = jnp.exp(scores - top_score)
        prob_total = lax.optimization_barrier(jnp.sum(probs, axis=-1))
        rounded = lax.optimization_barrier(probs.astype(jnp.bfloat16)).astype(jnp.float32)
        summed = jnp.einsum('kgts,skd->tkgd', rounded, values_expanded)
        return (summed / jnp.transpose(prob_total, (2, 0, 1))[..., None]).astype(jnp.bfloat16)
    heads_out = lax.map(attend, blocked_queries).reshape(token_total, QUERY_HEADS * HEAD_SIZE)
    group_width = QUERY_HEADS * HEAD_SIZE // N_TP
    mixed = jnp.zeros((token_total, D), jnp.float32)
    for group_index in range(N_TP):
        lower = group_index * group_width
        partial_value = jnp.dot(heads_out[:, lower:lower + group_width], out_proj[lower:lower + group_width], preferred_element_type=jnp.float32)
        mixed = mixed + lax.optimization_barrier(partial_value.astype(jnp.bfloat16)).astype(jnp.float32)
    mixed_rows = mixed.astype(jnp.bfloat16)
    count_b = mix_tokens.shape[0]
    blocks = count_b // TOK_B_DEV
    values_b = mix_tokens.astype(jnp.float32)
    normed = (values_b * lax.rsqrt(lax.optimization_barrier(jnp.mean(values_b * values_b, axis=-1, keepdims=True)) + EPS) * norm_gain).astype(jnp.bfloat16)
    flat = expert_ids.reshape(blocks, TOK_B_DEV * TOPK)
    onehot = (flat[..., None] == jnp.arange(EXPERTS, dtype=jnp.int32)).astype(jnp.int32)
    slots = lax.optimization_barrier(jnp.sum((jnp.cumsum(onehot, axis=1) - onehot) * onehot, axis=-1))
    owners = jnp.arange(blocks, dtype=jnp.int32)[:, None]
    places = ((flat * blocks + owners) * CAP + slots).reshape(count_b, TOPK).astype(jnp.int32)
    buffer = jnp.zeros((EXPERTS * blocks * CAP, D), jnp.bfloat16)
    for route_slot in range(TOPK):
        buffer = buffer.at[places[:, route_slot]].set(normed)
    stacked = buffer.reshape(EXPERTS, blocks * CAP, D)
    hidden_width = FFE // N_TP

    def run_expert(operands):
        expert_in, gate_w, up_w, down_w = operands
        gate_out = jnp.dot(expert_in, gate_w, preferred_element_type=jnp.float32)
        up_out = jnp.dot(expert_in, up_w, preferred_element_type=jnp.float32)
        active = (jax.nn.silu(gate_out) * up_out).astype(jnp.bfloat16)
        summed = jnp.zeros((expert_in.shape[0], D), jnp.float32)
        for group_index in range(N_TP):
            lower = group_index * hidden_width
            partial_value = jnp.dot(active[:, lower:lower + hidden_width], down_w[lower:lower + hidden_width], preferred_element_type=jnp.float32)
            summed = summed + lax.optimization_barrier(partial_value.astype(jnp.bfloat16)).astype(jnp.float32)
        return summed.astype(jnp.bfloat16)
    results = lax.map(run_expert, (stacked, gate_proj, up_proj, down_proj)).reshape(EXPERTS * blocks * CAP, D)
    first_weight = jax.nn.sigmoid(expert_score[:, 0] - expert_score[:, 1])
    combined = first_weight[:, None] * results[places[:, 0]].astype(jnp.float32) + (1.0 - first_weight)[:, None] * results[places[:, 1]].astype(jnp.float32)
    return (mixed_rows, combined.astype(jnp.bfloat16))
```

```python
import math

import jax
import jax.numpy as jnp
from jax import lax
from jax.sharding import PartitionSpec as P

GRID_W = 64


EPS = 1e-06
THETA = 10000.0


def head_norm(vectors, gain):
    return vectors * lax.rsqrt(jnp.mean(vectors * vectors, axis=-1, keepdims=True) + EPS) * gain


def rotate_grid(vectors, token_positions):
    length, heads, head_dim = vectors.shape
    quarter = head_dim // 4
    freqs = 1.0 / THETA ** (jnp.arange(quarter, dtype=jnp.float32) * 4.0 / head_dim)
    grid_row = (token_positions // GRID_W).astype(jnp.float32)
    grid_col = (token_positions % GRID_W).astype(jnp.float32)
    angles = jnp.stack([grid_row[:, None] * freqs, grid_col[:, None] * freqs], axis=1)
    cosine = jnp.cos(angles)[:, None]
    sine = jnp.sin(angles)[:, None]
    halves = vectors.reshape(length, heads, 2, 2, quarter)
    first = halves[..., 0, :]
    second = halves[..., 1, :]
    turned = jnp.stack([first * cosine - second * sine, second * cosine + first * sine], axis=-2)
    return turned.reshape(length, heads, head_dim)


def prepare_inputs(raw_rows, gain, heads, token_positions):
    length = raw_rows.shape[0]
    head_dim = gain.shape[0]
    vectors = raw_rows.astype(jnp.float32).reshape(length, heads, head_dim)
    return rotate_grid(head_norm(vectors, gain), token_positions).astype(jnp.bfloat16)


def mixer_half(query_rows, projected_keys, projected_values, query_gain, key_norm_gain, out_proj):
    length = query_rows.shape[0]
    head_dim = query_gain.shape[0]
    kv_heads = projected_keys.shape[1] // head_dim
    q_heads = query_rows.shape[1] // head_dim
    queries_per_group = q_heads // kv_heads
    token_positions = lax.axis_index("ep") * length + jnp.arange(length, dtype=jnp.int32)
    query_matrix = prepare_inputs(query_rows, query_gain, q_heads, token_positions).reshape(
        length, kv_heads, queries_per_group, head_dim
    )
    keys_turned = prepare_inputs(projected_keys, key_norm_gain, kv_heads, token_positions).reshape(
        length, kv_heads * head_dim
    )
    score_scale = head_dim ** (-0.5)
    initial = (
        jnp.full((kv_heads, queries_per_group, length), -1e30, jnp.float32),
        jnp.zeros((kv_heads, queries_per_group, length), jnp.float32),
        jnp.zeros((length, kv_heads, queries_per_group, head_dim), jnp.float32),
    )
    width = kv_heads * head_dim
    pair = lax.all_gather(
        jnp.concatenate([keys_turned, projected_values], axis=1), "ep", axis=0, tiled=True
    )
    key_piece = pair[:, :width]
    value_piece = pair[:, width:]
    piece_rows = key_piece.shape[0]
    step_rows = math.gcd(piece_rows, 1024)

    def one_block(block_index, running):
        run_max, run_sum, run_acc = running
        offset = block_index * step_rows
        key_block = lax.dynamic_slice_in_dim(key_piece, offset, step_rows, 0).reshape(
            step_rows, kv_heads, head_dim
        )
        value_block = lax.dynamic_slice_in_dim(value_piece, offset, step_rows, 0).reshape(
            step_rows, kv_heads, head_dim
        )
        scores = (
            jnp.einsum(
                "tkgd,skd->kgts", query_matrix, key_block, preferred_element_type=jnp.float32
            )
            * score_scale
        )
        new_max = jnp.maximum(run_max, jnp.max(scores, axis=-1))
        factor = jnp.exp(run_max - new_max)
        weights = jnp.exp(scores - new_max[..., None])
        run_sum = run_sum * factor + jnp.sum(weights, axis=-1)
        update = jnp.einsum(
            "kgts,skd->tkgd",
            weights.astype(jnp.bfloat16),
            value_block,
            preferred_element_type=jnp.float32,
        )
        run_acc = run_acc * jnp.transpose(factor, (2, 0, 1))[..., None] + update
        return (new_max, run_sum, run_acc)

    run_max, run_sum, run_acc = lax.fori_loop(0, piece_rows // step_rows, one_block, initial)
    heads_out = (
        (run_acc / jnp.transpose(run_sum, (2, 0, 1))[..., None])
        .astype(jnp.bfloat16)
        .reshape(length, q_heads * head_dim)
    )
    return jnp.dot(heads_out, out_proj, preferred_element_type=jnp.float32).astype(jnp.bfloat16)


def both_halves(
    query_rows,
    projected_keys,
    projected_values,
    query_gain,
    key_norm_gain,
    out_proj,
    mix_tokens,
    norm_gain,
    expert_ids,
    expert_score,
    gate_proj,
    up_proj,
    down_proj,
):
    length, model_dim = mix_tokens.shape
    top_count = expert_ids.shape[1]
    local_experts = gate_proj.shape[0]
    expert_axis = lax.axis_size("ep")
    experts_all = expert_axis * local_experts
    capacity = length * top_count * 3 // (2 * experts_all)
    values_b = mix_tokens.astype(jnp.float32)
    normed = (
        values_b
        * lax.rsqrt(jnp.mean(values_b * values_b, axis=-1, keepdims=True) + EPS)
        * norm_gain
    ).astype(jnp.bfloat16)
    flat = expert_ids.reshape(length * top_count)
    onehot = (flat[:, None] == jnp.arange(experts_all, dtype=jnp.int32)).astype(jnp.int32)
    slots = jnp.sum((jnp.cumsum(onehot, axis=0) - onehot) * onehot, axis=1)
    target = flat * capacity + slots
    placed = (target[:, None] == jnp.arange(experts_all * capacity, dtype=jnp.int32)).astype(
        jnp.int32
    )
    placed = jnp.sum(placed.reshape(length, top_count, experts_all * capacity), axis=1).astype(
        jnp.bfloat16
    )
    outgoing = jnp.einsum("re,rd->ed", placed, normed, preferred_element_type=jnp.float32).astype(
        jnp.bfloat16
    )
    outgoing = outgoing.reshape(expert_axis, local_experts, capacity, model_dim)
    arrived = lax.all_to_all(outgoing, "ep", split_axis=0, concat_axis=0, tiled=True)
    arrived, query_rows, projected_keys, projected_values = lax.optimization_barrier(
        (arrived, query_rows, projected_keys, projected_values)
    )
    rows_in = lax.all_gather(arrived, "tp", axis=0, tiled=True)
    head_partial = mixer_half(
        query_rows, projected_keys, projected_values, query_gain, key_norm_gain, out_proj
    )
    rows_in, head_partial = lax.optimization_barrier((rows_in, head_partial))
    mixed_rows = lax.psum_scatter(head_partial, "tp", scatter_dimension=0, tiled=True)
    gate_out = jnp.einsum("secd,edf->secf", rows_in, gate_proj, preferred_element_type=jnp.float32)
    up_out = jnp.einsum("secd,edf->secf", rows_in, up_proj, preferred_element_type=jnp.float32)
    active = (jax.nn.silu(gate_out) * up_out).astype(jnp.bfloat16)
    summed = lax.psum_scatter(
        jnp.einsum("secf,efd->secd", active, down_proj, preferred_element_type=jnp.float32).astype(
            jnp.bfloat16
        ),
        "tp",
        scatter_dimension=0,
        tiled=True,
    )
    returned = lax.all_to_all(summed, "ep", split_axis=0, concat_axis=0, tiled=True)
    results = returned.reshape(experts_all * capacity, model_dim)
    first_weight = jax.nn.sigmoid(expert_score[:, 0] - expert_score[:, 1])
    picks = target.reshape(length, top_count)
    chosen = [
        jnp.dot(
            (picks[:, k : k + 1] == jnp.arange(experts_all * capacity, dtype=jnp.int32)).astype(
                jnp.bfloat16
            ),
            results,
            preferred_element_type=jnp.float32,
        )
        for k in range(2)
    ]
    combined = first_weight[:, None] * chosen[0] + (1.0 - first_weight)[:, None] * chosen[1]
    return (mixed_rows, combined.astype(jnp.bfloat16))


def local(
    query_rows,
    projected_keys,
    projected_values,
    query_gain,
    key_norm_gain,
    out_proj,
    mix_tokens,
    norm_gain,
    expert_ids,
    expert_score,
    gate_proj,
    up_proj,
    down_proj,
):
    return both_halves(
        query_rows,
        projected_keys,
        projected_values,
        query_gain,
        key_norm_gain,
        out_proj,
        mix_tokens,
        norm_gain,
        expert_ids,
        expert_score,
        gate_proj,
        up_proj,
        down_proj,
    )


def solution(mesh):
    in_specs = (
        P(("grp", "ep"), "tp"),
        P(("grp", "ep"), "tp"),
        P(("grp", "ep"), "tp"),
        P(),
        P(),
        P("tp", None),
        P(("grp", "ep", "tp"), None),
        P(),
        P(("grp", "ep", "tp"), None),
        P(("grp", "ep", "tp"), None),
        P("ep", None, "tp"),
        P("ep", None, "tp"),
        P("ep", "tp", None),
    )
    out_specs = (P(("grp", "ep", "tp"), None), P(("grp", "ep", "tp"), None))
    return jax.shard_map(local, mesh=mesh, in_specs=in_specs, out_specs=out_specs, check_vma=False)
```

```python
import functools
import math

import jax
import jax.numpy as jnp
from jax import lax
from jax.experimental import pallas as pl
from jax.experimental.pallas import tpu as pltpu
from jax.sharding import PartitionSpec as P

GRID_W = 64


MESH = pl.DeviceIdType.MESH
EPS = 1e-06
THETA = 10000.0


def head_norm(vectors, gain):
    return vectors * lax.rsqrt(jnp.mean(vectors * vectors, axis=-1, keepdims=True) + EPS) * gain


def rotate_grid(vectors, token_positions):
    length, heads, head_dim = vectors.shape
    quarter = head_dim // 4
    freqs = 1.0 / THETA ** (jnp.arange(quarter, dtype=jnp.float32) * 4.0 / head_dim)
    grid_row = (token_positions // GRID_W).astype(jnp.float32)
    grid_col = (token_positions % GRID_W).astype(jnp.float32)
    angles = jnp.stack([grid_row[:, None] * freqs, grid_col[:, None] * freqs], axis=1)
    cosine = jnp.cos(angles)[:, None]
    sine = jnp.sin(angles)[:, None]
    halves = vectors.reshape(length, heads, 2, 2, quarter)
    first = halves[..., 0, :]
    second = halves[..., 1, :]
    turned = jnp.stack([first * cosine - second * sine, second * cosine + first * sine], axis=-2)
    return turned.reshape(length, heads, head_dim)


def prepare_inputs(raw_rows, gain, heads, token_positions):
    length = raw_rows.shape[0]
    head_dim = gain.shape[0]
    vectors = raw_rows.astype(jnp.float32).reshape(length, heads, head_dim)
    return rotate_grid(head_norm(vectors, gain), token_positions).astype(jnp.bfloat16)


def mixer_half(query_rows, projected_keys, projected_values, query_gain, key_norm_gain, out_proj):
    length = query_rows.shape[0]
    head_dim = query_gain.shape[0]
    kv_heads = projected_keys.shape[1] // head_dim
    q_heads = query_rows.shape[1] // head_dim
    queries_per_group = q_heads // kv_heads
    token_positions = lax.axis_index("ep") * length + jnp.arange(length, dtype=jnp.int32)
    query_matrix = prepare_inputs(query_rows, query_gain, q_heads, token_positions).reshape(
        length, kv_heads, queries_per_group, head_dim
    )
    keys_turned = prepare_inputs(projected_keys, key_norm_gain, kv_heads, token_positions).reshape(
        length, kv_heads * head_dim
    )
    score_scale = head_dim ** (-0.5)
    initial = (
        jnp.full((kv_heads, queries_per_group, length), -1e30, jnp.float32),
        jnp.zeros((kv_heads, queries_per_group, length), jnp.float32),
        jnp.zeros((length, kv_heads, queries_per_group, head_dim), jnp.float32),
    )
    width = kv_heads * head_dim
    pair = lax.all_gather(
        jnp.concatenate([keys_turned, projected_values], axis=1), "ep", axis=0, tiled=True
    )
    key_piece = pair[:, :width]
    value_piece = pair[:, width:]
    piece_rows = key_piece.shape[0]
    step_rows = math.gcd(piece_rows, 1024)

    def one_block(block_index, running):
        run_max, run_sum, run_acc = running
        offset = block_index * step_rows
        key_block = lax.dynamic_slice_in_dim(key_piece, offset, step_rows, 0).reshape(
            step_rows, kv_heads, head_dim
        )
        value_block = lax.dynamic_slice_in_dim(value_piece, offset, step_rows, 0).reshape(
            step_rows, kv_heads, head_dim
        )
        scores = (
            jnp.einsum(
                "tkgd,skd->kgts", query_matrix, key_block, preferred_element_type=jnp.float32
            )
            * score_scale
        )
        new_max = jnp.maximum(run_max, jnp.max(scores, axis=-1))
        factor = jnp.exp(run_max - new_max)
        weights = jnp.exp(scores - new_max[..., None])
        run_sum = run_sum * factor + jnp.sum(weights, axis=-1)
        update = jnp.einsum(
            "kgts,skd->tkgd",
            weights.astype(jnp.bfloat16),
            value_block,
            preferred_element_type=jnp.float32,
        )
        run_acc = run_acc * jnp.transpose(factor, (2, 0, 1))[..., None] + update
        return (new_max, run_sum, run_acc)

    run_max, run_sum, run_acc = lax.fori_loop(0, piece_rows // step_rows, one_block, initial)
    heads_out = (
        (run_acc / jnp.transpose(run_sum, (2, 0, 1))[..., None])
        .astype(jnp.bfloat16)
        .reshape(length, q_heads * head_dim)
    )
    return jnp.dot(heads_out, out_proj, preferred_element_type=jnp.float32).astype(jnp.bfloat16)


def flip(index, bits):
    result, place = 0, 1
    for _ in range(8):
        mine = (index // place) % 2
        result = result + place * ((1 - mine) if bits & place else mine)
        place *= 2
    return result


def exchange_kernel(
    steps,
    out_ref,
    gate_ref,
    up_ref,
    down_ref,
    back_ref,
    rows,
    act,
    part,
    from_core,
    to_x,
    from_x,
    total,
    zs,
    zr,
    xs,
    xr,
    cs,
    cr,
    ps,
    pr,
    qs,
    qr,
    bs,
    br,
):
    me = lax.axis_index("ep")
    lane = lax.axis_index("tp")
    peers = [flip(me, k) for k in range(steps)]
    core, across = flip(lane, 1), flip(lane, 2)
    cap, width = out_ref.shape[1], out_ref.shape[2]
    hidden = gate_ref.shape[1]
    tile = math.gcd(hidden, 256)
    tile_out = math.gcd(width, 256)

    barrier = pltpu.get_barrier_semaphore()
    friends = [{"ep": peers[k], "tp": lane} for k in range(1, steps)]
    friends += [{"ep": me, "tp": core}, {"ep": me, "tp": across}]
    for friend in friends:
        pl.semaphore_signal(barrier, inc=1, device_id=friend, device_id_type=MESH)
    pl.semaphore_wait(barrier, len(friends))

    def remote(src, dst, send, recv, ep_to, tp_to):
        return pltpu.make_async_remote_copy(
            src_ref=src,
            dst_ref=dst,
            send_sem=send,
            recv_sem=recv,
            device_id={"ep": ep_to, "tp": tp_to},
            device_id_type=MESH,
        )

    z_in = [None] + [
        remote(out_ref.at[peers[k]], rows.at[k, 0], zs.at[k], zr.at[k], peers[k], lane)
        for k in range(1, steps)
    ]
    x_in = [
        remote(
            out_ref.at[me] if k == 0 else rows.at[k, 0],
            rows.at[k, 1],
            xs.at[k],
            xr.at[k],
            me,
            across,
        )
        for k in range(steps)
    ]
    c_in = [
        remote(
            rows.at[k, pl.ds(0, 2)], rows.at[k, pl.ds(2, 2)], cs.at[k], cr.at[k], me, core
        )
        for k in range(steps)
    ]
    c_out = [
        remote(part.at[k, pl.ds(2, 2)], from_core.at[k], ps.at[k], pr.at[k], me, core)
        for k in range(steps)
    ]
    x_out = [
        remote(to_x.at[k], from_x.at[k], qs.at[k], qr.at[k], me, across) for k in range(steps)
    ]
    z_out = [None] + [
        remote(total.at[k], back_ref.at[me], bs.at[k], br.at[k], peers[k], lane)
        for k in range(1, steps)
    ]

    def stage_a(k):
        if k > 0:
            z_in[k].wait_recv()
        x_in[k].start()

    def stage_b(k):
        x_in[k].wait_recv()
        c_in[k].start()

    def stage_c(k):
        c_in[k].wait_recv()

        @pl.loop(0, hidden // tile)
        def _(i):
            cols = pl.ds(pl.multiple_of(i * tile, tile), tile)
            block = rows[k].reshape(4 * cap, width)
            gate = jnp.dot(block, gate_ref[:, cols], preferred_element_type=jnp.float32)
            up = jnp.dot(block, up_ref[:, cols], preferred_element_type=jnp.float32)
            act[:, cols] = (gate / (1.0 + jnp.exp(-gate)) * up).astype(jnp.bfloat16)

        @pl.loop(0, width // tile_out)
        def _(i):
            cols = pl.ds(pl.multiple_of(i * tile_out, tile_out), tile_out)
            summed = jnp.dot(act[...], down_ref[:, cols], preferred_element_type=jnp.float32)
            part[k, :, :, cols] = summed.astype(jnp.bfloat16).reshape(4, cap, tile_out)

        c_out[k].start()

    def stage_d(k):
        c_out[k].wait_recv()
        to_x[k] = (
            part[k, 1].astype(jnp.float32) + from_core[k, 1].astype(jnp.float32)
        ).astype(jnp.bfloat16)
        x_out[k].start()

    def stage_e(k):
        x_out[k].wait_recv()
        summed = (
            part[k, 0].astype(jnp.float32)
            + from_core[k, 0].astype(jnp.float32)
            + from_x[k].astype(jnp.float32)
        ).astype(jnp.bfloat16)
        if k == 0:
            back_ref[me] = summed
        else:
            total[k] = summed
            z_out[k].start()

    for k in range(1, steps):
        z_in[k].start()
    rows[0, 0] = out_ref[me]
    stage_a(0)
    stage_b(0)
    for k in range(steps):
        if k > 0:
            stage_d(k - 1)
        if k + 1 < steps:
            stage_a(k + 1)
        stage_c(k)
        if k > 0:
            stage_e(k - 1)
        if k + 1 < steps:
            stage_b(k + 1)
    stage_d(steps - 1)
    stage_e(steps - 1)
    for k in range(steps):
        if k > 0:
            z_out[k].wait_recv()
            z_in[k].wait_send()
            z_out[k].wait_send()
        for copy in (x_in[k], c_in[k], c_out[k], x_out[k]):
            copy.wait_send()


def exchange(outgoing, gate, up, down):
    steps, cap, width = outgoing.shape
    hidden = gate.shape[1]
    vmem = pl.BlockSpec(memory_space=pltpu.VMEM)
    kind = jnp.bfloat16
    return pl.pallas_call(
        functools.partial(exchange_kernel, steps),
        out_shape=jax.ShapeDtypeStruct((steps, cap, width), kind),
        in_specs=[vmem] * 4,
        out_specs=vmem,
        scratch_shapes=[
            pltpu.VMEM((steps, 4, cap, width), kind),
            pltpu.VMEM((4 * cap, hidden), kind),
            pltpu.VMEM((steps, 4, cap, width), kind),
            pltpu.VMEM((steps, 2, cap, width), kind),
            pltpu.VMEM((steps, cap, width), kind),
            pltpu.VMEM((steps, cap, width), kind),
            pltpu.VMEM((steps, cap, width), kind),
        ]
        + [pltpu.SemaphoreType.DMA((steps,))] * 12,
        compiler_params=pltpu.CompilerParams(
            collective_id=0, has_side_effects=True, vmem_limit_bytes=60 * 1024 * 1024
        ),
    )(outgoing, gate, up, down)


def fits_exchange(lanes, steps, local_experts, cap, width, hidden):
    blocks = 14 * steps * cap * width * 2 + 3 * width * hidden * 2
    return (
        lanes == 4
        and local_experts == 1
        and steps & (steps - 1) == 0
        and steps <= 8
        and cap % 16 == 0
        and blocks < 44 * 1024 * 1024
    )


def exchange_plain(outgoing, gate_proj, up_proj, down_proj):
    rows_in = lax.all_gather(
        lax.all_to_all(outgoing, "ep", split_axis=0, concat_axis=0, tiled=True),
        "tp",
        axis=0,
        tiled=True,
    )
    gate_out = jnp.einsum("secd,edf->secf", rows_in, gate_proj, preferred_element_type=jnp.float32)
    up_out = jnp.einsum("secd,edf->secf", rows_in, up_proj, preferred_element_type=jnp.float32)
    active = (jax.nn.silu(gate_out) * up_out).astype(jnp.bfloat16)
    summed = lax.psum_scatter(
        jnp.einsum("secf,efd->secd", active, down_proj, preferred_element_type=jnp.float32).astype(
            jnp.bfloat16
        ),
        "tp",
        scatter_dimension=0,
        tiled=True,
    )
    return lax.all_to_all(summed, "ep", split_axis=0, concat_axis=0, tiled=True)


def both_halves(
    query_rows,
    projected_keys,
    projected_values,
    query_gain,
    key_norm_gain,
    out_proj,
    mix_tokens,
    norm_gain,
    expert_ids,
    expert_score,
    gate_proj,
    up_proj,
    down_proj,
):
    length, model_dim = mix_tokens.shape
    top_count = expert_ids.shape[1]
    local_experts = gate_proj.shape[0]
    expert_axis = lax.axis_size("ep")
    experts_all = expert_axis * local_experts
    capacity = length * top_count * 3 // (2 * experts_all)
    values_b = mix_tokens.astype(jnp.float32)
    normed = (
        values_b
        * lax.rsqrt(jnp.mean(values_b * values_b, axis=-1, keepdims=True) + EPS)
        * norm_gain
    ).astype(jnp.bfloat16)
    flat = expert_ids.reshape(length * top_count)
    onehot = (flat[:, None] == jnp.arange(experts_all, dtype=jnp.int32)).astype(jnp.int32)
    slots = jnp.sum((jnp.cumsum(onehot, axis=0) - onehot) * onehot, axis=1)
    target = flat * capacity + slots
    placed = (target[:, None] == jnp.arange(experts_all * capacity, dtype=jnp.int32)).astype(
        jnp.int32
    )
    placed = jnp.sum(placed.reshape(length, top_count, experts_all * capacity), axis=1).astype(
        jnp.bfloat16
    )
    outgoing = jnp.einsum("re,rd->ed", placed, normed, preferred_element_type=jnp.float32).astype(
        jnp.bfloat16
    )
    outgoing = outgoing.reshape(expert_axis, local_experts, capacity, model_dim)
    head_partial = mixer_half(
        query_rows, projected_keys, projected_values, query_gain, key_norm_gain, out_proj
    )
    lanes = lax.axis_size("tp")
    pieces = lax.all_to_all(
        head_partial.reshape(lanes, -1, head_partial.shape[1]),
        "tp",
        split_axis=0,
        concat_axis=0,
        tiled=True,
    )
    mixed_rows = jnp.sum(pieces.astype(jnp.float32), axis=0).astype(jnp.bfloat16)
    if fits_exchange(
        lanes, expert_axis, local_experts, capacity, model_dim, gate_proj.shape[2]
    ):
        returned = exchange(
            outgoing.reshape(expert_axis, capacity, model_dim),
            gate_proj.reshape(gate_proj.shape[1:]),
            up_proj.reshape(up_proj.shape[1:]),
            down_proj.reshape(down_proj.shape[1:]),
        )
    else:
        returned = exchange_plain(outgoing, gate_proj, up_proj, down_proj)
    results = returned.reshape(experts_all * capacity, model_dim)
    first_weight = jax.nn.sigmoid(expert_score[:, 0] - expert_score[:, 1])
    picks = target.reshape(length, top_count)
    chosen = [
        jnp.dot(
            (picks[:, k : k + 1] == jnp.arange(experts_all * capacity, dtype=jnp.int32)).astype(
                jnp.bfloat16
            ),
            results,
            preferred_element_type=jnp.float32,
        )
        for k in range(2)
    ]
    combined = first_weight[:, None] * chosen[0] + (1.0 - first_weight)[:, None] * chosen[1]
    return (mixed_rows, combined.astype(jnp.bfloat16))


def local(
    query_rows,
    projected_keys,
    projected_values,
    query_gain,
    key_norm_gain,
    out_proj,
    mix_tokens,
    norm_gain,
    expert_ids,
    expert_score,
    gate_proj,
    up_proj,
    down_proj,
):
    return both_halves(
        query_rows,
        projected_keys,
        projected_values,
        query_gain,
        key_norm_gain,
        out_proj,
        mix_tokens,
        norm_gain,
        expert_ids,
        expert_score,
        gate_proj,
        up_proj,
        down_proj,
    )


def solution(mesh):
    in_specs = (
        P(("grp", "ep"), "tp"),
        P(("grp", "ep"), "tp"),
        P(("grp", "ep"), "tp"),
        P(),
        P(),
        P("tp", None),
        P(("grp", "ep", "tp"), None),
        P(),
        P(("grp", "ep", "tp"), None),
        P(("grp", "ep", "tp"), None),
        P("ep", None, "tp"),
        P("ep", None, "tp"),
        P("ep", "tp", None),
    )
    out_specs = (P(("grp", "ep", "tp"), None), P(("grp", "ep", "tp"), None))
    return jax.shard_map(local, mesh=mesh, in_specs=in_specs, out_specs=out_specs, check_vma=False)
```

```python
import functools
import math

import jax
import jax.numpy as jnp
from jax import lax
from jax.experimental import pallas as pl
from jax.experimental.pallas import tpu as pltpu
from jax.sharding import PartitionSpec as P

GRID_W = 64


MESH = pl.DeviceIdType.MESH
EPS = 1e-06
THETA = 10000.0


def head_norm(vectors, gain):
    return vectors * lax.rsqrt(jnp.mean(vectors * vectors, axis=-1, keepdims=True) + EPS) * gain


def rotate_grid(vectors, token_positions):
    length, heads, head_dim = vectors.shape
    quarter = head_dim // 4
    freqs = 1.0 / THETA ** (jnp.arange(quarter, dtype=jnp.float32) * 4.0 / head_dim)
    grid_row = (token_positions // GRID_W).astype(jnp.float32)
    grid_col = (token_positions % GRID_W).astype(jnp.float32)
    angles = jnp.stack([grid_row[:, None] * freqs, grid_col[:, None] * freqs], axis=1)
    cosine = jnp.cos(angles)[:, None]
    sine = jnp.sin(angles)[:, None]
    halves = vectors.reshape(length, heads, 2, 2, quarter)
    first = halves[..., 0, :]
    second = halves[..., 1, :]
    turned = jnp.stack([first * cosine - second * sine, second * cosine + first * sine], axis=-2)
    return turned.reshape(length, heads, head_dim)


def prepare_inputs(raw_rows, gain, heads, token_positions):
    length = raw_rows.shape[0]
    head_dim = gain.shape[0]
    vectors = raw_rows.astype(jnp.float32).reshape(length, heads, head_dim)
    return rotate_grid(head_norm(vectors, gain), token_positions).astype(jnp.bfloat16)


def mixer_prepare(query_rows, projected_keys, projected_values, query_gain, key_norm_gain):
    length = query_rows.shape[0]
    head_dim = query_gain.shape[0]
    kv_heads = projected_keys.shape[1] // head_dim
    q_heads = query_rows.shape[1] // head_dim
    token_positions = lax.axis_index("ep") * length + jnp.arange(length, dtype=jnp.int32)
    query_matrix = prepare_inputs(query_rows, query_gain, q_heads, token_positions).reshape(
        length, q_heads * head_dim
    )
    keys_turned = prepare_inputs(projected_keys, key_norm_gain, kv_heads, token_positions).reshape(
        length, kv_heads * head_dim
    )
    return query_matrix, jnp.concatenate([keys_turned, projected_values], axis=1)


def attend_plain(query_matrix, own_pair, head_dim):
    length = query_matrix.shape[0]
    kv_heads = own_pair.shape[1] // (2 * head_dim)
    q_heads = query_matrix.shape[1] // head_dim
    queries_per_group = q_heads // kv_heads
    query_matrix = query_matrix.reshape(length, kv_heads, queries_per_group, head_dim)
    score_scale = head_dim ** (-0.5)
    initial = (
        jnp.full((kv_heads, queries_per_group, length), -1e30, jnp.float32),
        jnp.zeros((kv_heads, queries_per_group, length), jnp.float32),
        jnp.zeros((length, kv_heads, queries_per_group, head_dim), jnp.float32),
    )
    width = kv_heads * head_dim
    pair = lax.all_gather(own_pair, "ep", axis=0, tiled=True)
    key_piece = pair[:, :width]
    value_piece = pair[:, width:]
    piece_rows = key_piece.shape[0]
    step_rows = math.gcd(piece_rows, 1024)

    def one_block(block_index, running):
        run_max, run_sum, run_acc = running
        offset = block_index * step_rows
        key_block = lax.dynamic_slice_in_dim(key_piece, offset, step_rows, 0).reshape(
            step_rows, kv_heads, head_dim
        )
        value_block = lax.dynamic_slice_in_dim(value_piece, offset, step_rows, 0).reshape(
            step_rows, kv_heads, head_dim
        )
        scores = (
            jnp.einsum(
                "tkgd,skd->kgts", query_matrix, key_block, preferred_element_type=jnp.float32
            )
            * score_scale
        )
        new_max = jnp.maximum(run_max, jnp.max(scores, axis=-1))
        factor = jnp.exp(run_max - new_max)
        weights = jnp.exp(scores - new_max[..., None])
        run_sum = run_sum * factor + jnp.sum(weights, axis=-1)
        update = jnp.einsum(
            "kgts,skd->tkgd",
            weights.astype(jnp.bfloat16),
            value_block,
            preferred_element_type=jnp.float32,
        )
        run_acc = run_acc * jnp.transpose(factor, (2, 0, 1))[..., None] + update
        return (new_max, run_sum, run_acc)

    run_max, run_sum, run_acc = lax.fori_loop(0, piece_rows // step_rows, one_block, initial)
    return (
        (run_acc / jnp.transpose(run_sum, (2, 0, 1))[..., None])
        .astype(jnp.bfloat16)
        .reshape(length, q_heads * head_dim)
    )


def flip(index, bits):
    result, place = 0, 1
    for _ in range(8):
        mine = (index // place) % 2
        result = result + place * ((1 - mine) if bits & place else mine)
        place *= 2
    return result


def exchange_kernel(
    steps,
    out_ref,
    gate_ref,
    up_ref,
    down_ref,
    query_ref,
    pair_ref,
    back_ref,
    heads_ref,
    rows,
    act,
    part,
    from_core,
    to_x,
    from_x,
    total,
    pairs,
    zs,
    zr,
    xs,
    xr,
    cs,
    cr,
    ps,
    pr,
    qs,
    qr,
    bs,
    br,
    ks,
    kr,
):
    me = lax.axis_index("ep")
    lane = lax.axis_index("tp")
    peers = [flip(me, k) for k in range(steps)]
    core, across = flip(lane, 1), flip(lane, 2)
    cap, width = out_ref.shape[1], out_ref.shape[2]
    hidden = gate_ref.shape[1]
    tile = math.gcd(hidden, 256)
    tile_out = math.gcd(width, 256)

    barrier = pltpu.get_barrier_semaphore()
    friends = [{"ep": peers[k], "tp": lane} for k in range(1, steps)]
    friends += [{"ep": me, "tp": core}, {"ep": me, "tp": across}]
    for friend in friends:
        pl.semaphore_signal(barrier, inc=1, device_id=friend, device_id_type=MESH)
    pl.semaphore_wait(barrier, len(friends))

    def remote(src, dst, send, recv, ep_to, tp_to):
        return pltpu.make_async_remote_copy(
            src_ref=src,
            dst_ref=dst,
            send_sem=send,
            recv_sem=recv,
            device_id={"ep": ep_to, "tp": tp_to},
            device_id_type=MESH,
        )

    z_in = [None] + [
        remote(out_ref.at[peers[k]], rows.at[k, 0], zs.at[k], zr.at[k], peers[k], lane)
        for k in range(1, steps)
    ]
    kv_in = [None] + [
        remote(pair_ref, pairs.at[k], ks.at[k], kr.at[k], peers[k], lane)
        for k in range(1, steps)
    ]
    x_in = [
        remote(
            out_ref.at[me] if k == 0 else rows.at[k, 0],
            rows.at[k, 1],
            xs.at[k],
            xr.at[k],
            me,
            across,
        )
        for k in range(steps)
    ]
    c_in = [
        remote(
            rows.at[k, pl.ds(0, 2)], rows.at[k, pl.ds(2, 2)], cs.at[k], cr.at[k], me, core
        )
        for k in range(steps)
    ]
    c_out = [
        remote(part.at[k, pl.ds(2, 2)], from_core.at[k], ps.at[k], pr.at[k], me, core)
        for k in range(steps)
    ]
    x_out = [
        remote(to_x.at[k], from_x.at[k], qs.at[k], qr.at[k], me, across) for k in range(steps)
    ]
    z_out = [None] + [
        remote(total.at[k], back_ref.at[me], bs.at[k], br.at[k], peers[k], lane)
        for k in range(1, steps)
    ]

    def stage_a(k):
        if k > 0:
            z_in[k].wait_recv()
        x_in[k].start()

    def stage_b(k):
        x_in[k].wait_recv()
        c_in[k].start()

    def stage_c(k):
        c_in[k].wait_recv()

        @pl.loop(0, hidden // tile)
        def _(i):
            cols = pl.ds(pl.multiple_of(i * tile, tile), tile)
            block = rows[k].reshape(4 * cap, width)
            gate = jnp.dot(block, gate_ref[:, cols], preferred_element_type=jnp.float32)
            up = jnp.dot(block, up_ref[:, cols], preferred_element_type=jnp.float32)
            act[:, cols] = (gate / (1.0 + jnp.exp(-gate)) * up).astype(jnp.bfloat16)

        @pl.loop(0, width // tile_out)
        def _(i):
            cols = pl.ds(pl.multiple_of(i * tile_out, tile_out), tile_out)
            summed = jnp.dot(act[...], down_ref[:, cols], preferred_element_type=jnp.float32)
            part[k, :, :, cols] = summed.astype(jnp.bfloat16).reshape(4, cap, tile_out)

        c_out[k].start()

    def stage_d(k):
        c_out[k].wait_recv()
        to_x[k] = (
            part[k, 1].astype(jnp.float32) + from_core[k, 1].astype(jnp.float32)
        ).astype(jnp.bfloat16)
        x_out[k].start()

    def stage_e(k):
        x_out[k].wait_recv()
        summed = (
            part[k, 0].astype(jnp.float32)
            + from_core[k, 0].astype(jnp.float32)
            + from_x[k].astype(jnp.float32)
        ).astype(jnp.bfloat16)
        if k == 0:
            back_ref[me] = summed
        else:
            total[k] = summed
            z_out[k].start()

    def attend():
        for k in range(1, steps):
            kv_in[k].wait_recv()
        held = steps * pair_ref.shape[0]
        dim = pair_ref.shape[1] // 2
        keys = pairs[:, :, :dim].reshape(held, dim)
        values = pairs[:, :, dim:].reshape(held, dim)
        for head in range(query_ref.shape[1] // dim):
            cols = slice(head * dim, (head + 1) * dim)
            scores = (
                lax.dot_general(
                    query_ref[:, cols],
                    keys,
                    (((1,), (1,)), ((), ())),
                    preferred_element_type=jnp.float32,
                )
                * dim ** (-0.5)
            )
            probs = jnp.exp(scores - jnp.max(scores, axis=-1, keepdims=True))
            amount = jnp.sum(probs, axis=-1, keepdims=True)
            summed = jnp.dot(
                probs.astype(jnp.bfloat16), values, preferred_element_type=jnp.float32
            )
            heads_ref[:, cols] = (summed / amount).astype(jnp.bfloat16)

    for k in range(1, steps):
        kv_in[k].start()
        z_in[k].start()
    rows[0, 0] = out_ref[me]
    pairs[0] = pair_ref[...]
    stage_a(0)
    stage_b(0)
    for k in range(steps):
        if k > 0:
            stage_d(k - 1)
        if k == 1:
            attend()
        if k + 1 < steps:
            stage_a(k + 1)
        stage_c(k)
        if k > 0:
            stage_e(k - 1)
        if k + 1 < steps:
            stage_b(k + 1)
    stage_d(steps - 1)
    stage_e(steps - 1)
    for k in range(steps):
        if k > 0:
            z_out[k].wait_recv()
            z_in[k].wait_send()
            kv_in[k].wait_send()
            z_out[k].wait_send()
        for copy in (x_in[k], c_in[k], c_out[k], x_out[k]):
            copy.wait_send()


def exchange(outgoing, gate, up, down, queries, pair):
    steps, cap, width = outgoing.shape
    hidden = gate.shape[1]
    vmem = pl.BlockSpec(memory_space=pltpu.VMEM)
    kind = jnp.bfloat16
    return pl.pallas_call(
        functools.partial(exchange_kernel, steps),
        out_shape=(
            jax.ShapeDtypeStruct((steps, cap, width), kind),
            jax.ShapeDtypeStruct(queries.shape, kind),
        ),
        in_specs=[vmem] * 6,
        out_specs=(vmem, vmem),
        scratch_shapes=[
            pltpu.VMEM((steps, 4, cap, width), kind),
            pltpu.VMEM((4 * cap, hidden), kind),
            pltpu.VMEM((steps, 4, cap, width), kind),
            pltpu.VMEM((steps, 2, cap, width), kind),
            pltpu.VMEM((steps, cap, width), kind),
            pltpu.VMEM((steps, cap, width), kind),
            pltpu.VMEM((steps, cap, width), kind),
            pltpu.VMEM((steps,) + pair.shape, kind),
        ]
        + [pltpu.SemaphoreType.DMA((steps,))] * 14,
        compiler_params=pltpu.CompilerParams(
            collective_id=0, has_side_effects=True, vmem_limit_bytes=60 * 1024 * 1024
        ),
    )(outgoing, gate, up, down, queries, pair)


def fits_exchange(lanes, steps, local_experts, cap, width, hidden, length, kv_heads):
    blocks = 14 * steps * cap * width * 2 + 3 * width * hidden * 2
    return (
        lanes == 4
        and local_experts == 1
        and steps & (steps - 1) == 0
        and 1 < steps <= 8
        and kv_heads == 1
        and length % 16 == 0
        and length <= 256
        and cap % 16 == 0
        and blocks < 44 * 1024 * 1024
    )


def exchange_plain(outgoing, gate_proj, up_proj, down_proj):
    rows_in = lax.all_gather(
        lax.all_to_all(outgoing, "ep", split_axis=0, concat_axis=0, tiled=True),
        "tp",
        axis=0,
        tiled=True,
    )
    gate_out = jnp.einsum("secd,edf->secf", rows_in, gate_proj, preferred_element_type=jnp.float32)
    up_out = jnp.einsum("secd,edf->secf", rows_in, up_proj, preferred_element_type=jnp.float32)
    active = (jax.nn.silu(gate_out) * up_out).astype(jnp.bfloat16)
    summed = lax.psum_scatter(
        jnp.einsum("secf,efd->secd", active, down_proj, preferred_element_type=jnp.float32).astype(
            jnp.bfloat16
        ),
        "tp",
        scatter_dimension=0,
        tiled=True,
    )
    return lax.all_to_all(summed, "ep", split_axis=0, concat_axis=0, tiled=True)


def both_halves(
    query_rows,
    projected_keys,
    projected_values,
    query_gain,
    key_norm_gain,
    out_proj,
    mix_tokens,
    norm_gain,
    expert_ids,
    expert_score,
    gate_proj,
    up_proj,
    down_proj,
):
    length, model_dim = mix_tokens.shape
    top_count = expert_ids.shape[1]
    local_experts = gate_proj.shape[0]
    expert_axis = lax.axis_size("ep")
    experts_all = expert_axis * local_experts
    capacity = length * top_count * 3 // (2 * experts_all)
    values_b = mix_tokens.astype(jnp.float32)
    normed = (
        values_b
        * lax.rsqrt(jnp.mean(values_b * values_b, axis=-1, keepdims=True) + EPS)
        * norm_gain
    ).astype(jnp.bfloat16)
    flat = expert_ids.reshape(length * top_count)
    onehot = (flat[:, None] == jnp.arange(experts_all, dtype=jnp.int32)).astype(jnp.int32)
    slots = jnp.sum((jnp.cumsum(onehot, axis=0) - onehot) * onehot, axis=1)
    target = flat * capacity + slots
    placed = (target[:, None] == jnp.arange(experts_all * capacity, dtype=jnp.int32)).astype(
        jnp.int32
    )
    placed = jnp.sum(placed.reshape(length, top_count, experts_all * capacity), axis=1).astype(
        jnp.bfloat16
    )
    outgoing = jnp.einsum("re,rd->ed", placed, normed, preferred_element_type=jnp.float32).astype(
        jnp.bfloat16
    )
    outgoing = outgoing.reshape(expert_axis, local_experts, capacity, model_dim)
    lanes = lax.axis_size("tp")
    head_dim = query_gain.shape[0]
    queries, pair = mixer_prepare(
        query_rows, projected_keys, projected_values, query_gain, key_norm_gain
    )
    if fits_exchange(
        lanes,
        expert_axis,
        local_experts,
        capacity,
        model_dim,
        gate_proj.shape[2],
        queries.shape[0],
        pair.shape[1] // (2 * head_dim),
    ):
        returned, heads_out = exchange(
            outgoing.reshape(expert_axis, capacity, model_dim),
            gate_proj.reshape(gate_proj.shape[1:]),
            up_proj.reshape(up_proj.shape[1:]),
            down_proj.reshape(down_proj.shape[1:]),
            queries,
            pair,
        )
    else:
        heads_out = attend_plain(queries, pair, head_dim)
        returned = exchange_plain(outgoing, gate_proj, up_proj, down_proj)
    head_partial = jnp.dot(heads_out, out_proj, preferred_element_type=jnp.float32).astype(
        jnp.bfloat16
    )
    pieces = lax.all_to_all(
        head_partial.reshape(lanes, -1, head_partial.shape[1]),
        "tp",
        split_axis=0,
        concat_axis=0,
        tiled=True,
    )
    mixed_rows = jnp.sum(pieces.astype(jnp.float32), axis=0).astype(jnp.bfloat16)
    results = returned.reshape(experts_all * capacity, model_dim)
    first_weight = jax.nn.sigmoid(expert_score[:, 0] - expert_score[:, 1])
    picks = target.reshape(length, top_count)
    chosen = [
        jnp.dot(
            (picks[:, k : k + 1] == jnp.arange(experts_all * capacity, dtype=jnp.int32)).astype(
                jnp.bfloat16
            ),
            results,
            preferred_element_type=jnp.float32,
        )
        for k in range(2)
    ]
    combined = first_weight[:, None] * chosen[0] + (1.0 - first_weight)[:, None] * chosen[1]
    return (mixed_rows, combined.astype(jnp.bfloat16))


def local(
    query_rows,
    projected_keys,
    projected_values,
    query_gain,
    key_norm_gain,
    out_proj,
    mix_tokens,
    norm_gain,
    expert_ids,
    expert_score,
    gate_proj,
    up_proj,
    down_proj,
):
    return both_halves(
        query_rows,
        projected_keys,
        projected_values,
        query_gain,
        key_norm_gain,
        out_proj,
        mix_tokens,
        norm_gain,
        expert_ids,
        expert_score,
        gate_proj,
        up_proj,
        down_proj,
    )


def solution(mesh):
    in_specs = (
        P(("grp", "ep"), "tp"),
        P(("grp", "ep"), "tp"),
        P(("grp", "ep"), "tp"),
        P(),
        P(),
        P("tp", None),
        P(("grp", "ep", "tp"), None),
        P(),
        P(("grp", "ep", "tp"), None),
        P(("grp", "ep", "tp"), None),
        P("ep", None, "tp"),
        P("ep", None, "tp"),
        P("ep", "tp", None),
    )
    out_specs = (P(("grp", "ep", "tp"), None), P(("grp", "ep", "tp"), None))
    return jax.shard_map(local, mesh=mesh, in_specs=in_specs, out_specs=out_specs, check_vma=False)
```
